32 devices in a mesh: sp: 16 (over z, y, core), tp: 2 (over x).
Axes of the slice: x: 2, y: 2, z: 4, core: 2. Of those that a mesh axis runs over, the one named last changes fastest.
Arguments:
- resid: bfloat16 [4096, 2048], P('sp', 'tp'), may hold values from -80 to 80, as said below
- norm_gain: float32 [2, 2048], P(None, 'tp'), may hold values from 0.1 to 1.9
- w_in: bfloat16 [2, 2048, 1024], P(None, 'tp', 'sp'), may hold values from -0.125 to 0.125
- w_pool: bfloat16 [2, 4, 256, 256], P(None, 'tp'), may hold values from -0.375 to 0.375
- pool_scale: float32 [2, 1024], P(None, 'tp'), may hold values from 0.1 to 1.9
- w_out: bfloat16 [2, 1024, 2048], P(None, 'sp', 'tp'), may hold values from -0.1875 to 0.1875
- final_gain: float32 [2048], P('tp'), may hold values from 0.1 to 1.9
Outputs:
- normed: bfloat16 [4096, 2048], P('sp', 'tp')
The draws below stay inside these ranges and needn't reach their ends.
Inputs may be any that keep to these rules, and one draw needn't show every extreme that they name: `resid`: Real-valued entries of order 0.1 to ten.
All inputs are finite; a program needn't handle non-finite values.
Results may differ from the reference program's by a relative error of at most 0.015.
Values may be sent and summed in bfloat16 or wider, within the bound.
A program may use at most 64 MiB of HBM per device.

```python
import jax
import jax.numpy as jnp
from jax import lax

D = 2048
GROUPS = 4
CG = 256
LAYERS = 2
POOL = 1024
TOKENS = 4096
N_TP = 2


def draw_resid(key, part):
    keys = jax.random.split(jax.random.fold_in(key, 11), 3)
    row_scale = 10.0 ** jax.random.uniform(keys[0], (TOKENS, 1), jnp.float32, -0.5, 0.5)
    position = jnp.arange(D, dtype=jnp.float32) / D
    jitter = jnp.exp(jax.random.uniform(keys[1], (1, D), jnp.float32, -0.35, 0.35))
    col_scale = (10.0 ** (position - 0.5))[None, :] * jitter
    base = jnp.clip(jax.random.normal(keys[2], (TOKENS, D), jnp.float32), -4.0, 4.0)
    return (base * row_scale * col_scale).astype(jnp.bfloat16)


def block_levels(key, dims, cuts, least, top_value):
    def one(dim, shards_of):
        heights = jax.random.uniform(jax.random.fold_in(jax.random.fold_in(key, 6), dim), (shards_of,), jnp.float32, least / len(cuts), top_value / len(cuts))
        return jnp.repeat(jnp.exp(heights), dims[dim] // shards_of).reshape((-1,) + (1,) * (len(dims) - dim - 1))

    loudness = one(*cuts[0])
    for cut in cuts[1:]:
        loudness = loudness * one(*cut)
    return loudness


def scatter_about(stream_key, extent, spread, most, cuts=(), kind=jnp.bfloat16):
    factor_of = block_levels(stream_key, extent, cuts, -0.22, 0.18) if cuts else 1.0
    values = jax.random.normal(stream_key, extent, jnp.float32) * spread * factor_of
    return jnp.minimum(jnp.maximum(values, -most), most).astype(kind)


def setup_inputs(seed: int = 0) -> dict:
    seeds = jax.random.split(jax.random.key(seed), 8)
    resid = draw_resid(jax.random.fold_in(seeds[7], 71), 0)
    norm_gain = jnp.clip(1.0 + 0.18 * jax.random.normal(seeds[1], (LAYERS, D), jnp.float32), 0.1, 1.9)
    w_in = scatter_about(seeds[2], (LAYERS, D, POOL), D ** -0.5, 0.125, ((1, 2), (2, 16)))
    w_pool = scatter_about(seeds[3], (LAYERS, GROUPS, CG, CG), CG ** -0.5, 0.375, ((1, 2),))
    pool_scale = jnp.clip(1.0 + 0.18 * jax.random.normal(seeds[4], (LAYERS, POOL), jnp.float32), 0.1, 1.9)
    w_out = scatter_about(seeds[5], (LAYERS, POOL, D), POOL ** -0.5, 0.1875, ((1, 16), (2, 2)))
    final_gain = jnp.clip(1.0 + 0.18 * jax.random.normal(seeds[6], (D,), jnp.float32), 0.1, 1.9)
    return {"resid": resid, "norm_gain": norm_gain, "w_in": w_in, "w_pool": w_pool, "pool_scale": pool_scale, "w_out": w_out, "final_gain": final_gain}


margin = 8
eps = 1e-06

def nested_sums(padded, count_rows):
    total = padded[margin - 1:margin - 1 + count_rows] + padded[margin:margin + count_rows]
    sums = [total]
    for level in range(1, 4):
        half = 2 ** level
        for offset in range(half // 2 + 1, half + 1):
            total = total + padded[margin - offset:margin - offset + count_rows]
        for offset in range(half // 2, half):
            total = total + padded[margin + offset:margin + offset + count_rows]
        sums.append(total)
    return sums

def window_count(where, seq_len, level):
    left = 2 ** level
    right = 2 ** level - 1
    upper = jnp.clip(where + right + 1, 0, seq_len)
    lower = jnp.clip(where - left, 0, seq_len)
    return (upper - lower).astype(jnp.float32)

def scaled(xf, gain):
    squares = lax.optimization_barrier(jnp.sum(xf * xf, axis=1))
    return (xf * lax.rsqrt(squares / D + eps)[:, None] * gain[None, :]).astype(jnp.bfloat16)

def reference(resid, norm_gain, w_in, w_pool, pool_scale, w_out, final_gain):
    where = jnp.arange(TOKENS, dtype=jnp.int32)
    block = D // N_TP
    xf = resid.astype(jnp.float32)
    for layer in range(LAYERS):
        hidden = scaled(xf, norm_gain[layer])
        total = jnp.zeros((TOKENS, POOL), jnp.float32)
        for span_index in range(N_TP):
            part = jnp.dot(hidden[:, span_index * block:(span_index + 1) * block], w_in[layer, span_index * block:(span_index + 1) * block], preferred_element_type=jnp.float32).astype(jnp.bfloat16)
            part = lax.optimization_barrier(part)
            total = total + part.astype(jnp.float32)
        upward = total.astype(jnp.bfloat16)
        upward_f = upward.astype(jnp.float32)
        pieces = []
        for group in range(GROUPS):
            cols = upward_f[:, group * CG:(group + 1) * CG]
            padded = jnp.pad(cols, ((margin, margin), (0, 0)))
            wsum = nested_sums(padded, TOKENS)[group]
            counted = window_count(where, TOKENS, group)
            pooled = (wsum / counted[:, None] - cols).astype(jnp.bfloat16)
            mapped = jnp.dot(pooled, w_pool[layer, group], preferred_element_type=jnp.float32)
            pieces.append(mapped * pool_scale[layer, group * CG:(group + 1) * CG][None, :])
        mixed = jnp.concatenate(pieces, axis=1).astype(jnp.bfloat16)
        output = jnp.dot(mixed, w_out[layer], preferred_element_type=jnp.float32)
        stored = (xf + output).astype(jnp.bfloat16)
        stored = lax.optimization_barrier(stored)
        xf = stored.astype(jnp.float32)
    return scaled(xf, final_gain)
```

```python
import functools

import jax
import jax.numpy as jnp
from jax import lax
from jax.experimental import pallas as pl
from jax.experimental.pallas import tpu as pltpu
from jax.sharding import PartitionSpec as P

LAYERS = 2


margin = 8
eps = 1e-06


def padded_2(value, sides, width):
    for axis, dim in sides:
        count, length = (lax.axis_size(axis), value.shape[dim])
        up = [(i, (i + 1) % count) for i in range(count - 1)]
        down = [(j, i) for i, j in up]
        last = lax.slice_in_dim(value, length - width, length, axis=dim)
        initial = lax.slice_in_dim(value, 0, width, axis=dim)
        before = lax.ppermute(last, axis, up)
        after = lax.ppermute(initial, axis, down)
        value = jnp.concatenate([before, value, after], axis=dim)
    return value


def nested_sums(padded, count_rows):
    total = padded[margin - 1 : margin - 1 + count_rows] + padded[margin : margin + count_rows]
    sums = [total]
    for level in range(1, 4):
        half = 2**level
        for offset in range(half // 2 + 1, half + 1):
            total = total + padded[margin - offset : margin - offset + count_rows]
        for offset in range(half // 2, half):
            total = total + padded[margin + offset : margin + offset + count_rows]
        sums.append(total)
    return sums


def window_count(where, seq_len, level):
    left = 2**level
    right = 2**level - 1
    upper = jnp.clip(where + right + 1, 0, seq_len)
    lower = jnp.clip(where - left, 0, seq_len)
    return (upper - lower).astype(jnp.float32)


def scaled(xf, gain, width):
    squares = lax.psum(jnp.sum(xf * xf, axis=1), "tp")
    return (xf * lax.rsqrt(squares / width + eps)[:, None] * gain[None, :]).astype(jnp.bfloat16)


def shards(resid, norm_gain, w_in, w_pool, pool_scale, w_out, final_gain):
    tok_rows = resid.shape[0]
    blocks_tp = lax.axis_size("tp")
    width = blocks_tp * resid.shape[1]
    channels = w_pool.shape[1] * w_pool.shape[2]
    groups_here = w_pool.shape[1]
    group_width = w_pool.shape[2]
    seq_len = tok_rows * lax.axis_size("sp")
    where = lax.axis_index("sp") * tok_rows + jnp.arange(tok_rows, dtype=jnp.int32)
    group_ids = (
        lax.axis_index("tp") * groups_here + jnp.arange(channels, dtype=jnp.int32) // group_width
    )
    all_in, all_out = (
        lax.all_gather(w_in, "sp", axis=2, tiled=True),
        lax.all_gather(w_out, "sp", axis=1, tiled=True),
    )
    xf = resid.astype(jnp.float32)
    for layer in range(LAYERS):
        own_hidden = scaled(xf, norm_gain[layer], width)
        in_block = all_in[layer]
        partial_value = jnp.dot(own_hidden, in_block, preferred_element_type=jnp.float32).astype(
            jnp.bfloat16
        )
        upward = (
            lax.psum_scatter(partial_value, "tp", scatter_dimension=1, tiled=True)
            .astype(jnp.float32)
            .astype(jnp.bfloat16)
        )
        padded = padded_2(upward, (("sp", 0),), margin).astype(jnp.float32)
        sums = nested_sums(padded, tok_rows)
        wsum = sums[0]
        counted = jnp.broadcast_to(window_count(where, seq_len, 0)[:, None], (tok_rows, channels))
        for level in range(1, 4):
            chosen = (group_ids == level)[None, :]
            wsum = jnp.where(chosen, sums[level], wsum)
            counted = jnp.where(chosen, window_count(where, seq_len, level)[:, None], counted)
        pooled = (wsum / counted - upward.astype(jnp.float32)).astype(jnp.bfloat16)
        mapped = jnp.einsum(
            "tgc,gcd->tgd",
            pooled.reshape(tok_rows, groups_here, group_width),
            w_pool[layer],
            preferred_element_type=jnp.float32,
        )
        mixed = (mapped.reshape(tok_rows, channels) * pool_scale[layer][None, :]).astype(
            jnp.bfloat16
        )
        mixed_all = lax.all_gather(mixed, "tp", axis=1, tiled=True)
        output = jnp.dot(mixed_all, all_out[layer], preferred_element_type=jnp.float32)
        stored = (xf + output).astype(jnp.bfloat16)
        stored = lax.optimization_barrier(stored)
        xf = stored.astype(jnp.float32)
    return scaled(xf, final_gain, width)


MESH = pl.DeviceIdType.MESH


def fused(
    sp_size,
    resid_ref,
    gain_ref,
    final_ref,
    own_w,
    pool_ref,
    pscale_ref,
    out_ref,
    weights,
    xg,
    xcur,
    own_part,
    acc,
    part_send,
    part_recv,
    uhalo,
    mix_send,
    mix_recv,
    ss_send,
    ss_recv,
    w_send_sem,
    w_recv_sem,
    x_send_sem,
    x_recv_sem,
    h_send_sem,
    h_recv_sem,
    s_send_sem,
    s_recv_sem,
):
    depth = sp_size // 4
    rows = own_w.shape[1]
    tokens, width_here = resid_ref.shape
    groups, cg = pool_ref.shape[1], pool_ref.shape[2]
    half = groups * cg
    width = 2 * width_here
    edge = 2 * margin
    me = lax.axis_index("sp")
    t = lax.axis_index("tp")
    peer = 1 - t
    core = lax.rem(me, 2)
    y = lax.rem(me // 2, 2)
    z = me // 4

    def number(zz, yy, cc):
        return (zz * 2 + yy) * 2 + cc

    sibling = number(z, y, 1 - core)
    across = number(z, 1 - y, core)

    barrier = pltpu.get_barrier_semaphore()

    def greet(device):
        pl.semaphore_signal(barrier, inc=1, device_id=device, device_id_type=MESH)

    greet({"sp": sibling})
    greet({"sp": across})
    greet({"tp": peer})
    for ok, who in (
        (z > 0, me - 4),
        (z < depth - 1, me + 4),
        (me > 0, me - 1),
        (me < sp_size - 1, me + 1),
    ):

        @pl.when(ok)
        def _(who=who):
            greet({"sp": who})

    expected = (
        3
        + jnp.where(z > 0, 1, 0)
        + jnp.where(z < depth - 1, 1, 0)
        + jnp.where(me > 0, 1, 0)
        + jnp.where(me < sp_size - 1, 1, 0)
    )
    pl.semaphore_wait(barrier, expected)

    def landing(stage, piece):
        return weights.at[stage, pl.ds(pl.multiple_of(piece * rows, rows), rows), :]

    def hop(stage, zz, yy, way, target, from_own=False):
        piece = number(zz, yy, core)
        slot = {"sib": zz * 2 + yy, "y": 2 * depth + zz, "up": 3 * depth + zz, "down": 4 * depth + zz}[way]
        return pltpu.make_async_remote_copy(
            src_ref=own_w.at[stage] if from_own else landing(stage, piece),
            dst_ref=landing(stage, piece),
            send_sem=w_send_sem.at[stage, slot],
            recv_sem=w_recv_sem.at[stage, piece],
            device_id={"sp": target},
            device_id_type=MESH,
        )

    def wait_piece(stage, zz, yy, cc):
        piece = number(zz, yy, cc)
        pltpu.make_async_remote_copy(
            src_ref=landing(stage, piece),
            dst_ref=landing(stage, piece),
            send_sem=w_send_sem.at[stage, 0],
            recv_sem=w_recv_sem.at[stage, piece],
            device_id={"sp": sibling},
            device_id_type=MESH,
        ).wait_recv()

    def each_own(stage, act):
        @pl.when(z < depth - 1)
        def _():
            act(hop(stage, z, y, "up", me + 4, True))

        @pl.when(z > 0)
        def _():
            act(hop(stage, z, y, "down", me - 4, True))

        act(hop(stage, z, y, "y", across, True))
        act(hop(stage, z, y, "sib", sibling, True))

    def each_z(stage, d, act, arrive):
        @pl.when(z - d >= 0)
        def _():
            if arrive:
                wait_piece(stage, z - d, y, core)

            @pl.when(z < depth - 1)
            def _():
                act(hop(stage, z - d, y, "up", me + 4))

            act(hop(stage, z - d, y, "y", across))
            act(hop(stage, z - d, y, "sib", sibling))

        @pl.when(z + d < depth)
        def _():
            if arrive:
                wait_piece(stage, z + d, y, core)

            @pl.when(z > 0)
            def _():
                act(hop(stage, z + d, y, "down", me - 4))

            act(hop(stage, z + d, y, "y", across))
            act(hop(stage, z + d, y, "sib", sibling))

    def each_y(stage, d, act, arrive):
        def one(zz):
            if arrive:
                wait_piece(stage, zz, 1 - y, core)
            act(hop(stage, zz, 1 - y, "sib", sibling))

        if d == 0:
            one(z)
        else:

            @pl.when(z - d >= 0)
            def _():
                one(z - d)

            @pl.when(z + d < depth)
            def _():
                one(z + d)

    begin = lambda copy: copy.start()
    drain = lambda copy: copy.wait_send()

    def process(stage):
        for d in range(1, depth):
            each_z(stage, d, begin, True)
            if d == depth - 1 and stage + 1 < 2 * LAYERS:
                each_own(stage + 1, begin)
            each_y(stage, d - 1, begin, True)
        each_y(stage, depth - 1, begin, True)

    def settle(stage):
        for zz in range(depth):
            for yy in range(2):
                wait_piece(stage, zz, yy, 1 - core)

    def finish(stage):
        each_own(stage, drain)
        for d in range(1, depth):
            each_z(stage, d, drain, False)
        for d in range(depth):
            each_y(stage, d, drain, False)

    diagonal = lax.broadcasted_iota(jnp.int32, (tokens, tokens), 0) == lax.broadcasted_iota(
        jnp.int32, (tokens, tokens), 1
    )

    def send_squares(k):
        return pltpu.make_async_remote_copy(
            src_ref=ss_send.at[k],
            dst_ref=ss_recv.at[k],
            send_sem=s_send_sem.at[k],
            recv_sem=s_recv_sem.at[k],
            device_id={"tp": peer},
            device_id_type=MESH,
        )

    def store_squares(k, column):
        line = jnp.sum(jnp.where(diagonal, column, 0.0), axis=0, keepdims=True)
        ss_send[k] = jnp.broadcast_to(line, ss_send.shape[1:])

    def norm_factor(k):
        send_squares(k).wait_recv()
        line = ss_send[k][0:1, :] + ss_recv[k][0:1, :]
        column = jnp.sum(jnp.where(diagonal, line, 0.0), axis=1, keepdims=True)
        return lax.rsqrt(column / width + eps)

    def x_copy(kind, layer, j):
        k = (kind * LAYERS + layer) * groups + j
        source, target = ((part_send, part_recv), (mix_send, mix_recv))[kind]
        return pltpu.make_async_remote_copy(
            src_ref=source.at[layer, j],
            dst_ref=target.at[layer, j],
            send_sem=x_send_sem.at[k],
            recv_sem=x_recv_sem.at[k],
            device_id={"tp": peer},
            device_id_type=MESH,
        )

    def halo(layer, upward):
        if upward:
            source = uhalo.at[layer, pl.ds(tokens, edge), :]
            target = uhalo.at[layer, pl.ds(0, edge), :]
        else:
            source = uhalo.at[layer, pl.ds(edge, edge), :]
            target = uhalo.at[layer, pl.ds(edge + tokens, edge), :]
        k = layer * 2 + (1 if upward else 0)
        return pltpu.make_async_remote_copy(
            src_ref=source,
            dst_ref=target,
            send_sem=h_send_sem.at[k],
            recv_sem=h_recv_sem.at[k],
            device_id={"sp": me + 1 if upward else me - 1},
            device_id_type=MESH,
        )

    def project(layer, which, j):
        start = pl.multiple_of(which * half + j * cg, cg)
        block = weights[2 * layer, pl.ds(start, cg), :]
        return lax.dot_general(
            xg[...], block, (((1,), (1,)), ((), ())), preferred_element_type=jnp.float32
        )

    def inward(layer):
        for j in range(groups):
            part_send[layer, j] = project(layer, peer, j).astype(jnp.bfloat16)
        for j in range(groups):
            x_copy(0, layer, j).start()
            own_part[:, j * cg : (j + 1) * cg] = project(layer, t, j)

    def pooling(layer):
        factor = norm_factor(layer)
        for j in range(groups):
            x_copy(0, layer, j).wait_recv()
            value = own_part[:, j * cg : (j + 1) * cg] + part_recv[layer, j].astype(jnp.float32)
            uhalo[layer, pl.ds(edge, tokens), j * cg : (j + 1) * cg] = (value * factor).astype(
                jnp.bfloat16
            )
        row = lax.broadcasted_iota(jnp.int32, (tokens, tokens + 2 * edge), 0)
        col = lax.broadcasted_iota(jnp.int32, (tokens, tokens + 2 * edge), 1) - edge
        where = me * tokens + lax.broadcasted_iota(jnp.int32, (tokens, 1), 0)
        seq_len = tokens * sp_size

        @pl.when(me < sp_size - 1)
        def _():
            halo(layer, True).start()

        @pl.when(me > 0)
        def _():
            halo(layer, False).start()

        @pl.when(me == 0)
        def _():
            uhalo[layer, pl.ds(0, edge), :] = jnp.zeros((edge, half), jnp.bfloat16)

        @pl.when(me == sp_size - 1)
        def _():
            uhalo[layer, pl.ds(edge + tokens, edge), :] = jnp.zeros((edge, half), jnp.bfloat16)

        @pl.when(me > 0)
        def _():
            halo(layer, True).wait_recv()

        @pl.when(me < sp_size - 1)
        def _():
            halo(layer, False).wait_recv()

        for j in range(groups):
            left = jnp.left_shift(1, t * groups + j)
            band = jnp.where((col >= row - left) & (col <= row + left - 1), 1.0, 0.0).astype(
                jnp.bfloat16
            )
            cols = slice(j * cg, (j + 1) * cg)
            wsum = jnp.dot(band, uhalo[layer, :, cols], preferred_element_type=jnp.float32)
            upper = jnp.minimum(where + left, seq_len)
            lower = jnp.maximum(where - left, 0)
            counted = (upper - lower).astype(jnp.float32)
            pooled = wsum / counted - uhalo[layer, pl.ds(edge, tokens), cols].astype(jnp.float32)
            mapped = jnp.dot(
                pooled.astype(jnp.bfloat16), pool_ref[layer, j], preferred_element_type=jnp.float32
            )
            mix_send[layer, j] = (mapped * pscale_ref[layer : layer + 1, cols]).astype(jnp.bfloat16)
            if j > 0:
                x_copy(1, layer, j - 1).start()
        return lambda: x_copy(1, layer, groups - 1).start()

    step = cg

    def outward_own(layer):
        for n in range(0, width_here, step):
            total = None
            for j in range(groups):
                start = pl.multiple_of(t * half + j * cg, cg)
                block = weights[2 * layer + 1, pl.ds(start, cg), n : n + step]
                term = jnp.dot(mix_send[layer, j], block, preferred_element_type=jnp.float32)
                total = term if total is None else total + term
            acc[:, n : n + step] = total + xcur[:, n : n + step].astype(jnp.float32)

    def outward_peer(layer):
        squares = jnp.zeros((tokens, 1), jnp.float32)
        for j in range(groups):
            x_copy(1, layer, j).wait_recv()
        for n in range(0, width_here, step):
            total = acc[:, n : n + step]
            for j in range(groups):
                start = pl.multiple_of(peer * half + j * cg, cg)
                block = weights[2 * layer + 1, pl.ds(start, cg), n : n + step]
                total = total + jnp.dot(
                    mix_recv[layer, j], block, preferred_element_type=jnp.float32
                )
            stored = total.astype(jnp.bfloat16)
            xcur[:, n : n + step] = stored
            value = stored.astype(jnp.float32)
            squares = squares + jnp.sum(value * value, axis=1, keepdims=True)
            if layer + 1 < LAYERS:
                xg[:, n : n + step] = (
                    value * gain_ref[layer + 1 : layer + 2, n : n + step]
                ).astype(jnp.bfloat16)
        store_squares(layer + 1, squares)

    each_own(0, begin)
    squares = jnp.zeros((tokens, 1), jnp.float32)
    for n in range(0, width_here, step):
        value = resid_ref[:, n : n + step].astype(jnp.float32)
        squares = squares + jnp.sum(value * value, axis=1, keepdims=True)
        xcur[:, n : n + step] = resid_ref[:, n : n + step]
        xg[:, n : n + step] = (value * gain_ref[0:1, n : n + step]).astype(jnp.bfloat16)
    store_squares(0, squares)
    for stage in range(2 * LAYERS):
        weights[stage, pl.ds(pl.multiple_of(me * rows, rows), rows), :] = own_w[stage]
    send_squares(0).start()

    process(0)
    settle(0)
    for layer in range(LAYERS):
        inward(layer)
        process(2 * layer + 1)
        last = pooling(layer)
        last()
        settle(2 * layer + 1)
        outward_own(layer)
        if layer + 1 < LAYERS:
            process(2 * layer + 2)
        outward_peer(layer)
        if layer + 1 < LAYERS:
            settle(2 * layer + 2)
        send_squares(layer + 1).start()
    for stage in range(2 * LAYERS):
        finish(stage)
    for kind in range(2):
        for layer in range(LAYERS):
            for j in range(groups):
                x_copy(kind, layer, j).wait_send()
    for layer in range(LAYERS):

        @pl.when(me < sp_size - 1)
        def _(layer=layer):
            halo(layer, True).wait_send()

        @pl.when(me > 0)
        def _(layer=layer):
            halo(layer, False).wait_send()

    factor = norm_factor(LAYERS)
    for n in range(0, width_here, step):
        out_ref[:, n : n + step] = (
            xcur[:, n : n + step].astype(jnp.float32) * factor * final_ref[0:1, n : n + step]
        ).astype(jnp.bfloat16)
    for k in range(LAYERS + 1):
        send_squares(k).wait_send()


def one_kernel(resid, norm_gain, w_in, w_pool, pool_scale, w_out, final_gain):
    sp_size = lax.axis_size("sp")
    depth = sp_size // 4
    tokens, width_here = resid.shape
    rows = w_out.shape[1]
    groups, cg = w_pool.shape[1], w_pool.shape[2]
    half = groups * cg
    edge = 2 * margin
    turned = jnp.swapaxes(w_in, 1, 2)
    pieces = jnp.stack([turned, w_out], axis=1).reshape(2 * LAYERS, rows, width_here)
    vmem = pl.BlockSpec(memory_space=pltpu.VMEM)
    bf, f32 = jnp.bfloat16, jnp.float32
    dma = pltpu.SemaphoreType.DMA
    crossing = pltpu.VMEM((LAYERS, groups, tokens, cg), bf)
    return pl.pallas_call(
        functools.partial(fused, sp_size),
        out_shape=jax.ShapeDtypeStruct(resid.shape, bf),
        in_specs=[vmem] * 6,
        out_specs=vmem,
        scratch_shapes=[
            pltpu.VMEM((2 * LAYERS, sp_size * rows, width_here), bf),
            pltpu.VMEM((tokens, width_here), bf),
            pltpu.VMEM((tokens, width_here), bf),
            pltpu.VMEM((tokens, half), f32),
            pltpu.VMEM((tokens, width_here), f32),
            crossing,
            crossing,
            pltpu.VMEM((LAYERS, tokens + 2 * edge, half), bf),
            crossing,
            crossing,
            pltpu.VMEM((LAYERS + 1, 8, tokens), f32),
            pltpu.VMEM((LAYERS + 1, 8, tokens), f32),
            dma((2 * LAYERS, 5 * depth)),
            dma((2 * LAYERS, sp_size)),
            dma((2 * LAYERS * groups,)),
            dma((2 * LAYERS * groups,)),
            dma((2 * LAYERS,)),
            dma((2 * LAYERS,)),
            dma((LAYERS + 1,)),
            dma((LAYERS + 1,)),
        ],
        compiler_params=pltpu.CompilerParams(
            collective_id=0, has_side_effects=True, vmem_limit_bytes=48 * 2**20
        ),
    )(resid, norm_gain, final_gain[None, :], pieces, w_pool, pool_scale)


def spread(*args):
    resid, w_pool, w_out = args[0], args[3], args[5]
    fits = (
        lax.axis_size("tp") == 2
        and lax.axis_size("sp") % 4 == 0
        and w_out.shape[1] % 16 == 0
        and resid.shape[0] % 128 == 0
        and w_pool.shape[2] % 128 == 0
        and resid.shape[1] % w_pool.shape[2] == 0
    )
    return one_kernel(*args) if fits else shards(*args)


def solution(mesh):
    placed = (
        P("sp", "tp"),
        P(None, "tp"),
        P(None, "tp", "sp"),
        P(None, "tp", None, None),
        P(None, "tp"),
        P(None, "sp", "tp"),
        P("tp"),
    )
    return jax.shard_map(
        spread, mesh=mesh, in_specs=placed, out_specs=P("sp", "tp"), check_vma=False
    )
```

```python
import functools

import jax
import jax.numpy as jnp
from jax import lax
from jax.experimental import pallas as pl
from jax.experimental.pallas import tpu as pltpu
from jax.sharding import PartitionSpec as P

LAYERS = 2


margin = 8
eps = 1e-06


def padded_2(value, sides, width):
    for axis, dim in sides:
        count, length = (lax.axis_size(axis), value.shape[dim])
        up = [(i, (i + 1) % count) for i in range(count - 1)]
        down = [(j, i) for i, j in up]
        last = lax.slice_in_dim(value, length - width, length, axis=dim)
        initial = lax.slice_in_dim(value, 0, width, axis=dim)
        before = lax.ppermute(last, axis, up)
        after = lax.ppermute(initial, axis, down)
        value = jnp.concatenate([before, value, after], axis=dim)
    return value


def nested_sums(padded, count_rows):
    total = padded[margin - 1 : margin - 1 + count_rows] + padded[margin : margin + count_rows]
    sums = [total]
    for level in range(1, 4):
        half = 2**level
        for offset in range(half // 2 + 1, half + 1):
            total = total + padded[margin - offset : margin - offset + count_rows]
        for offset in range(half // 2, half):
            total = total + padded[margin + offset : margin + offset + count_rows]
        sums.append(total)
    return sums


def window_count(where, seq_len, level):
    left = 2**level
    right = 2**level - 1
    upper = jnp.clip(where + right + 1, 0, seq_len)
    lower = jnp.clip(where - left, 0, seq_len)
    return (upper - lower).astype(jnp.float32)


def scaled(xf, gain, width):
    squares = lax.psum(jnp.sum(xf * xf, axis=1), "tp")
    return (xf * lax.rsqrt(squares / width + eps)[:, None] * gain[None, :]).astype(jnp.bfloat16)


def shards(resid, norm_gain, w_in, w_pool, pool_scale, w_out, final_gain):
    tok_rows = resid.shape[0]
    blocks_tp = lax.axis_size("tp")
    width = blocks_tp * resid.shape[1]
    channels = w_pool.shape[1] * w_pool.shape[2]
    groups_here = w_pool.shape[1]
    group_width = w_pool.shape[2]
    seq_len = tok_rows * lax.axis_size("sp")
    where = lax.axis_index("sp") * tok_rows + jnp.arange(tok_rows, dtype=jnp.int32)
    group_ids = (
        lax.axis_index("tp") * groups_here + jnp.arange(channels, dtype=jnp.int32) // group_width
    )
    all_in, all_out = (
        lax.all_gather(w_in, "sp", axis=2, tiled=True),
        lax.all_gather(w_out, "sp", axis=1, tiled=True),
    )
    xf = resid.astype(jnp.float32)
    for layer in range(LAYERS):
        own_hidden = scaled(xf, norm_gain[layer], width)
        in_block = all_in[layer]
        partial_value = jnp.dot(own_hidden, in_block, preferred_element_type=jnp.float32).astype(
            jnp.bfloat16
        )
        upward = (
            lax.psum_scatter(partial_value, "tp", scatter_dimension=1, tiled=True)
            .astype(jnp.float32)
            .astype(jnp.bfloat16)
        )
        padded = padded_2(upward, (("sp", 0),), margin).astype(jnp.float32)
        sums = nested_sums(padded, tok_rows)
        wsum = sums[0]
        counted = jnp.broadcast_to(window_count(where, seq_len, 0)[:, None], (tok_rows, channels))
        for level in range(1, 4):
            chosen = (group_ids == level)[None, :]
            wsum = jnp.where(chosen, sums[level], wsum)
            counted = jnp.where(chosen, window_count(where, seq_len, level)[:, None], counted)
        pooled = (wsum / counted - upward.astype(jnp.float32)).astype(jnp.bfloat16)
        mapped = jnp.einsum(
            "tgc,gcd->tgd",
            pooled.reshape(tok_rows, groups_here, group_width),
            w_pool[layer],
            preferred_element_type=jnp.float32,
        )
        mixed = (mapped.reshape(tok_rows, channels) * pool_scale[layer][None, :]).astype(
            jnp.bfloat16
        )
        mixed_all = lax.all_gather(mixed, "tp", axis=1, tiled=True)
        output = jnp.dot(mixed_all, all_out[layer], preferred_element_type=jnp.float32)
        stored = (xf + output).astype(jnp.bfloat16)
        stored = lax.optimization_barrier(stored)
        xf = stored.astype(jnp.float32)
    return scaled(xf, final_gain, width)


MESH = pl.DeviceIdType.MESH


def fused(
    sp_size,
    resid_ref,
    gain_ref,
    final_ref,
    own_w,
    pool_ref,
    pscale_ref,
    out_ref,
    weights,
    xg,
    xcur,
    own_part,
    acc,
    part_send,
    part_recv,
    uhalo,
    mix_send,
    mix_recv,
    ss_send,
    ss_recv,
    w_send_sem,
    w_recv_sem,
    x_send_sem,
    x_recv_sem,
    h_send_sem,
    h_recv_sem,
    s_send_sem,
    s_recv_sem,
):
    depth = sp_size // 4
    rows = own_w.shape[1]
    tokens, width_here = resid_ref.shape
    groups, cg = pool_ref.shape[1], pool_ref.shape[2]
    half = groups * cg
    width = 2 * width_here
    edge = 2 * margin
    me = lax.axis_index("sp")
    t = lax.axis_index("tp")
    peer = 1 - t
    core = lax.rem(me, 2)
    y = lax.rem(me // 2, 2)
    z = me // 4

    def number(zz, yy, cc):
        return (zz * 2 + yy) * 2 + cc

    sibling = number(z, y, 1 - core)
    across = number(z, 1 - y, core)

    barrier = pltpu.get_barrier_semaphore()

    def greet(device):
        pl.semaphore_signal(barrier, inc=1, device_id=device, device_id_type=MESH)

    greet({"sp": sibling})
    greet({"sp": across})
    greet({"tp": peer})
    for ok, who in (
        (z > 0, me - 4),
        (z < depth - 1, me + 4),
        (z > 1, me - 8),
        (z < depth - 2, me + 8),
        (me > 0, me - 1),
        (me < sp_size - 1, me + 1),
    ):

        @pl.when(ok)
        def _(who=who):
            greet({"sp": who})

    expected = (
        3
        + jnp.where(z > 0, 1, 0)
        + jnp.where(z < depth - 1, 1, 0)
        + jnp.where(z > 1, 1, 0)
        + jnp.where(z < depth - 2, 1, 0)
        + jnp.where(me > 0, 1, 0)
        + jnp.where(me < sp_size - 1, 1, 0)
    )
    pl.semaphore_wait(barrier, expected)

    def landing(stage, piece):
        return weights.at[stage, pl.ds(pl.multiple_of(piece * rows, rows), rows), :]

    def hop(stage, zz, yy, way, target, from_own=False):
        piece = number(zz, yy, core)
        slot = {
            "sib": zz * 2 + yy,
            "y": 2 * depth + zz,
            "up1": 3 * depth + zz,
            "down1": 4 * depth + zz,
            "up2": 5 * depth,
            "down2": 5 * depth + 1,
            "pair": 5 * depth + 2,
        }[way]
        return pltpu.make_async_remote_copy(
            src_ref=own_w.at[stage] if from_own else landing(stage, piece),
            dst_ref=landing(stage, piece),
            send_sem=w_send_sem.at[stage, slot],
            recv_sem=w_recv_sem.at[stage, piece],
            device_id={"sp": target},
            device_id_type=MESH,
        )

    def wait_piece(stage, zz, yy, cc):
        piece = number(zz, yy, cc)
        pltpu.make_async_remote_copy(
            src_ref=landing(stage, piece),
            dst_ref=landing(stage, piece),
            send_sem=w_send_sem.at[stage, 0],
            recv_sem=w_recv_sem.at[stage, piece],
            device_id={"sp": sibling},
            device_id_type=MESH,
        ).wait_recv()

    def each_own(stage, act):
        for d in (2, 1):

            @pl.when(z + d < depth)
            def _(d=d):
                act(hop(stage, z, y, f"up{d}", me + 4 * d, True))

            @pl.when(z - d >= 0)
            def _(d=d):
                act(hop(stage, z, y, f"down{d}", me - 4 * d, True))

        act(hop(stage, z, y, "sib", sibling, True))

    def own_y(stage, act):
        act(hop(stage, z, y, "y", across, True))

    zpair = z + 1 - 2 * lax.rem(z, 2)
    by_pair = (core == 1) & (zpair < depth)

    def each_z(stage, d, act, arrive):
        @pl.when(z - d >= 0)
        def _():
            if arrive:
                wait_piece(stage, z - d, y, core)
            if d >= 2:

                @pl.when(z < depth - 1)
                def _():
                    act(hop(stage, z - d, y, "up1", me + 4))

            if d > 1:
                act(hop(stage, z - d, y, "y", across))
            else:

                @pl.when(jnp.logical_not(by_pair & (zpair == z - 1)))
                def _():
                    act(hop(stage, z - 1, y, "y", across))

            act(hop(stage, z - d, y, "sib", sibling))

        @pl.when(z + d < depth)
        def _():
            if arrive:
                wait_piece(stage, z + d, y, core)
            if d >= 2:

                @pl.when(z > 0)
                def _():
                    act(hop(stage, z + d, y, "down1", me - 4))

            if d > 1:
                act(hop(stage, z + d, y, "y", across))
            else:

                @pl.when(jnp.logical_not(by_pair & (zpair == z + 1)))
                def _():
                    act(hop(stage, z + 1, y, "y", across))

            act(hop(stage, z + d, y, "sib", sibling))

    def each_y(stage, d, act, arrive):
        def one(zz):
            if arrive:
                wait_piece(stage, zz, 1 - y, core)
            act(hop(stage, zz, 1 - y, "sib", sibling))

        if d == 0:
            one(z)

            @pl.when(by_pair)
            def _():
                act(hop(stage, z, 1 - y, "pair", number(zpair, y, core)))

        else:

            @pl.when(z - d >= 0)
            def _():
                one(z - d)

            @pl.when(z + d < depth)
            def _():
                one(z + d)

    begin = lambda copy: copy.start()
    drain = lambda copy: copy.wait_send()

    def step_own(stage):
        if stage < 2 * LAYERS:
            each_own(stage, begin)
        if stage + 1 < 2 * LAYERS:
            own_y(stage + 1, begin)

    def step_z(stage, d):
        if stage < 2 * LAYERS and d < depth:
            each_z(stage, d, begin, True)

    def step_y(stage, d):
        if stage < 2 * LAYERS and d < depth:
            each_y(stage, d, begin, True)

    def opening(stage):
        step_y(stage, 0)
        step_z(stage, 2)
        step_own(stage + 2)
        step_y(stage, 1)

    def closing(stage, ahead=True):
        for d in range(3, depth):
            step_z(stage, d)
        if ahead:
            step_z(stage + 1, 1)
        for d in range(2, depth):
            step_y(stage, d)
        if not ahead:
            step_z(stage + 1, 1)

    def settle(stage):
        for zz in range(depth):
            for yy in range(2):
                wait_piece(stage, zz, yy, 1 - core)

    def finish(stage):
        each_own(stage, drain)
        own_y(stage, drain)
        for d in range(1, depth):
            each_z(stage, d, drain, False)
        for d in range(depth):
            each_y(stage, d, drain, False)

    diagonal = lax.broadcasted_iota(jnp.int32, (tokens, tokens), 0) == lax.broadcasted_iota(
        jnp.int32, (tokens, tokens), 1
    )

    def send_squares(k):
        return pltpu.make_async_remote_copy(
            src_ref=ss_send.at[k],
            dst_ref=ss_recv.at[k],
            send_sem=s_send_sem.at[k],
            recv_sem=s_recv_sem.at[k],
            device_id={"tp": peer},
            device_id_type=MESH,
        )

    def store_squares(k, column):
        line = jnp.sum(jnp.where(diagonal, column, 0.0), axis=0, keepdims=True)
        ss_send[k] = jnp.broadcast_to(line, ss_send.shape[1:])

    def norm_factor(k):
        send_squares(k).wait_recv()
        line = ss_send[k][0:1, :] + ss_recv[k][0:1, :]
        column = jnp.sum(jnp.where(diagonal, line, 0.0), axis=1, keepdims=True)
        return lax.rsqrt(column / width + eps)

    def x_copy(kind, layer, j):
        k = (kind * LAYERS + layer) * groups + j
        source, target = ((part_send, part_recv), (mix_send, mix_recv))[kind]
        return pltpu.make_async_remote_copy(
            src_ref=source.at[layer, j],
            dst_ref=target.at[layer, j],
            send_sem=x_send_sem.at[k],
            recv_sem=x_recv_sem.at[k],
            device_id={"tp": peer},
            device_id_type=MESH,
        )

    def halo(layer, j, upward):
        if upward:
            source = uhalo.at[layer, j, pl.ds(tokens, edge), :]
            target = uhalo.at[layer, j, pl.ds(0, edge), :]
        else:
            source = uhalo.at[layer, j, pl.ds(edge, edge), :]
            target = uhalo.at[layer, j, pl.ds(edge + tokens, edge), :]
        k = (layer * groups + j) * 2 + (1 if upward else 0)
        return pltpu.make_async_remote_copy(
            src_ref=source,
            dst_ref=target,
            send_sem=h_send_sem.at[k],
            recv_sem=h_recv_sem.at[k],
            device_id={"sp": me + 1 if upward else me - 1},
            device_id_type=MESH,
        )

    def each_halo(layer, j, act):
        @pl.when(me < sp_size - 1)
        def _():
            act(halo(layer, j, True))

        @pl.when(me > 0)
        def _():
            act(halo(layer, j, False))

    def project(layer, which, j):
        start = pl.multiple_of(which * half + j * cg, cg)
        block = weights[2 * layer, pl.ds(start, cg), :]
        return lax.dot_general(
            xg[...], block, (((1,), (1,)), ((), ())), preferred_element_type=jnp.float32
        )

    def inward(layer):
        for j in range(groups):
            part_send[layer, j] = project(layer, peer, j).astype(jnp.bfloat16)
        for j in range(groups):
            x_copy(0, layer, j).start()
            own_part[:, j * cg : (j + 1) * cg] = project(layer, t, j)

    def pooling(layer):
        factor = norm_factor(layer)
        for j in range(groups):
            x_copy(0, layer, j).wait_recv()
            value = own_part[:, j * cg : (j + 1) * cg] + part_recv[layer, j].astype(jnp.float32)
            uhalo[layer, j, pl.ds(edge, tokens), :] = (value * factor).astype(jnp.bfloat16)
            each_halo(layer, j, begin)
        row = lax.broadcasted_iota(jnp.int32, (tokens, tokens + 2 * edge), 0)
        col = lax.broadcasted_iota(jnp.int32, (tokens, tokens + 2 * edge), 1) - edge
        where = me * tokens + lax.broadcasted_iota(jnp.int32, (tokens, 1), 0)
        seq_len = tokens * sp_size
        for j in range(groups):
            left = jnp.left_shift(1, t * groups + j)
            band = jnp.where((col >= row - left) & (col <= row + left - 1), 1.0, 0.0).astype(
                jnp.bfloat16
            )
            upper = jnp.minimum(where + left, seq_len)
            lower = jnp.maximum(where - left, 0)
            inverse = 1.0 / (upper - lower).astype(jnp.float32)

            @pl.when(me > 0)
            def _(j=j):
                halo(layer, j, True).wait_recv()

            @pl.when(me < sp_size - 1)
            def _(j=j):
                halo(layer, j, False).wait_recv()

            wsum = jnp.dot(band, uhalo[layer, j], preferred_element_type=jnp.float32)
            pooled = wsum * inverse - uhalo[layer, j, pl.ds(edge, tokens), :].astype(jnp.float32)
            mapped = jnp.dot(
                pooled.astype(jnp.bfloat16), pool_ref[layer, j], preferred_element_type=jnp.float32
            )
            scale = pscale_ref[layer : layer + 1, j * cg : (j + 1) * cg]
            mix_send[layer, j] = (mapped * scale).astype(jnp.bfloat16)
            x_copy(1, layer, j).start()

    step = cg

    def outward_own(layer):
        for n in range(0, width_here, step):
            total = None
            for j in range(groups):
                start = pl.multiple_of(t * half + j * cg, cg)
                block = weights[2 * layer + 1, pl.ds(start, cg), n : n + step]
                term = jnp.dot(mix_send[layer, j], block, preferred_element_type=jnp.float32)
                total = term if total is None else total + term
            acc[:, n : n + step] = total + xcur[:, n : n + step].astype(jnp.float32)

    def outward_peer(layer):
        squares = jnp.zeros((tokens, 1), jnp.float32)
        for j in range(groups):
            x_copy(1, layer, j).wait_recv()
        for n in range(0, width_here, step):
            total = acc[:, n : n + step]
            for j in range(groups):
                start = pl.multiple_of(peer * half + j * cg, cg)
                block = weights[2 * layer + 1, pl.ds(start, cg), n : n + step]
                total = total + jnp.dot(
                    mix_recv[layer, j], block, preferred_element_type=jnp.float32
                )
            stored = total.astype(jnp.bfloat16)
            xcur[:, n : n + step] = stored
            value = stored.astype(jnp.float32)
            squares = squares + jnp.sum(value * value, axis=1, keepdims=True)
            if layer + 1 < LAYERS:
                xg[:, n : n + step] = (
                    value * gain_ref[layer + 1 : layer + 2, n : n + step]
                ).astype(jnp.bfloat16)
        store_squares(layer + 1, squares)

    own_y(0, begin)
    step_own(0)
    step_own(1)
    squares = jnp.zeros((tokens, 1), jnp.float32)
    for n in range(0, width_here, step):
        value = resid_ref[:, n : n + step].astype(jnp.float32)
        squares = squares + jnp.sum(value * value, axis=1, keepdims=True)
        xcur[:, n : n + step] = resid_ref[:, n : n + step]
        xg[:, n : n + step] = (value * gain_ref[0:1, n : n + step]).astype(jnp.bfloat16)
    store_squares(0, squares)
    nothing = jnp.zeros((LAYERS, groups, edge, cg), jnp.bfloat16)

    @pl.when(me == 0)
    def _():
        uhalo[:, :, pl.ds(0, edge), :] = nothing

    @pl.when(me == sp_size - 1)
    def _():
        uhalo[:, :, pl.ds(edge + tokens, edge), :] = nothing

    for stage in range(2 * LAYERS):
        weights[stage, pl.ds(pl.multiple_of(me * rows, rows), rows), :] = own_w[stage]
    send_squares(0).start()

    step_z(0, 1)
    opening(0)
    closing(0, False)
    settle(0)
    for layer in range(LAYERS):
        inward(layer)
        opening(2 * layer + 1)
        pooling(layer)
        closing(2 * layer + 1)
        settle(2 * layer + 1)
        outward_own(layer)
        if layer + 1 < LAYERS:
            opening(2 * layer + 2)
        outward_peer(layer)
        send_squares(layer + 1).start()
        if layer + 1 < LAYERS:
            closing(2 * layer + 2)
            settle(2 * layer + 2)
    for stage in range(2 * LAYERS):
        finish(stage)
    for kind in range(2):
        for layer in range(LAYERS):
            for j in range(groups):
                x_copy(kind, layer, j).wait_send()
    for layer in range(LAYERS):
        for j in range(groups):
            each_halo(layer, j, drain)

    factor = norm_factor(LAYERS)
    for n in range(0, width_here, step):
        out_ref[:, n : n + step] = (
            xcur[:, n : n + step].astype(jnp.float32) * factor * final_ref[0:1, n : n + step]
        ).astype(jnp.bfloat16)
    for k in range(LAYERS + 1):
        send_squares(k).wait_send()


def one_kernel(resid, norm_gain, w_in, w_pool, pool_scale, w_out, final_gain):
    sp_size = lax.axis_size("sp")
    depth = sp_size // 4
    tokens, width_here = resid.shape
    rows = w_out.shape[1]
    groups, cg = w_pool.shape[1], w_pool.shape[2]
    half = groups * cg
    edge = 2 * margin
    turned = jnp.swapaxes(w_in, 1, 2)
    pieces = jnp.stack([turned, w_out], axis=1).reshape(2 * LAYERS, rows, width_here)
    vmem = pl.BlockSpec(memory_space=pltpu.VMEM)
    bf, f32 = jnp.bfloat16, jnp.float32
    dma = pltpu.SemaphoreType.DMA
    crossing = pltpu.VMEM((LAYERS, groups, tokens, cg), bf)
    return pl.pallas_call(
        functools.partial(fused, sp_size),
        out_shape=jax.ShapeDtypeStruct(resid.shape, bf),
        in_specs=[vmem] * 6,
        out_specs=vmem,
        scratch_shapes=[
            pltpu.VMEM((2 * LAYERS, sp_size * rows, width_here), bf),
            pltpu.VMEM((tokens, width_here), bf),
            pltpu.VMEM((tokens, width_here), bf),
            pltpu.VMEM((tokens, half), f32),
            pltpu.VMEM((tokens, width_here), f32),
            crossing,
            crossing,
            pltpu.VMEM((LAYERS, groups, tokens + 2 * edge, cg), bf),
            crossing,
            crossing,
            pltpu.VMEM((LAYERS + 1, 8, tokens), f32),
            pltpu.VMEM((LAYERS + 1, 8, tokens), f32),
            dma((2 * LAYERS, 5 * depth + 3)),
            dma((2 * LAYERS, sp_size)),
            dma((2 * LAYERS * groups,)),
            dma((2 * LAYERS * groups,)),
            dma((2 * LAYERS * groups,)),
            dma((2 * LAYERS * groups,)),
            dma((LAYERS + 1,)),
            dma((LAYERS + 1,)),
        ],
        compiler_params=pltpu.CompilerParams(
            collective_id=0, has_side_effects=True, vmem_limit_bytes=48 * 2**20
        ),
    )(resid, norm_gain, final_gain[None, :], pieces, w_pool, pool_scale)


def spread(*args):
    resid, w_pool, w_out = args[0], args[3], args[5]
    fits = (
        lax.axis_size("tp") == 2
        and lax.axis_size("sp") % 4 == 0
        and w_out.shape[1] % 16 == 0
        and resid.shape[0] % 128 == 0
        and w_pool.shape[2] % 128 == 0
        and resid.shape[1] % w_pool.shape[2] == 0
    )
    return one_kernel(*args) if fits else shards(*args)


def solution(mesh):
    placed = (
        P("sp", "tp"),
        P(None, "tp"),
        P(None, "tp", "sp"),
        P(None, "tp", None, None),
        P(None, "tp"),
        P(None, "sp", "tp"),
        P("tp"),
    )
    return jax.shard_map(
        spread, mesh=mesh, in_specs=placed, out_specs=P("sp", "tp"), check_vma=False
    )
```

```python
import functools

import jax
import jax.numpy as jnp
from jax import lax
from jax.experimental import pallas as pl
from jax.experimental.pallas import tpu as pltpu
from jax.sharding import PartitionSpec as P

LAYERS = 2


margin = 8
eps = 1e-06


def padded_2(value, sides, width):
    for axis, dim in sides:
        count, length = (lax.axis_size(axis), value.shape[dim])
        up = [(i, (i + 1) % count) for i in range(count - 1)]
        down = [(j, i) for i, j in up]
        last = lax.slice_in_dim(value, length - width, length, axis=dim)
        initial = lax.slice_in_dim(value, 0, width, axis=dim)
        before = lax.ppermute(last, axis, up)
        after = lax.ppermute(initial, axis, down)
        value = jnp.concatenate([before, value, after], axis=dim)
    return value


def nested_sums(padded, count_rows):
    total = padded[margin - 1 : margin - 1 + count_rows] + padded[margin : margin + count_rows]
    sums = [total]
    for level in range(1, 4):
        half = 2**level
        for offset in range(half // 2 + 1, half + 1):
            total = total + padded[margin - offset : margin - offset + count_rows]
        for offset in range(half // 2, half):
            total = total + padded[margin + offset : margin + offset + count_rows]
        sums.append(total)
    return sums


def window_count(where, seq_len, level):
    left = 2**level
    right = 2**level - 1
    upper = jnp.clip(where + right + 1, 0, seq_len)
    lower = jnp.clip(where - left, 0, seq_len)
    return (upper - lower).astype(jnp.float32)


def scaled(xf, gain, width):
    squares = lax.psum(jnp.sum(xf * xf, axis=1), "tp")
    return (xf * lax.rsqrt(squares / width + eps)[:, None] * gain[None, :]).astype(jnp.bfloat16)


def shards(resid, norm_gain, w_in, w_pool, pool_scale, w_out, final_gain):
    tok_rows = resid.shape[0]
    blocks_tp = lax.axis_size("tp")
    width = blocks_tp * resid.shape[1]
    channels = w_pool.shape[1] * w_pool.shape[2]
    groups_here = w_pool.shape[1]
    group_width = w_pool.shape[2]
    seq_len = tok_rows * lax.axis_size("sp")
    where = lax.axis_index("sp") * tok_rows + jnp.arange(tok_rows, dtype=jnp.int32)
    group_ids = (
        lax.axis_index("tp") * groups_here + jnp.arange(channels, dtype=jnp.int32) // group_width
    )
    all_in, all_out = (
        lax.all_gather(w_in, "sp", axis=2, tiled=True),
        lax.all_gather(w_out, "sp", axis=1, tiled=True),
    )
    xf = resid.astype(jnp.float32)
    for layer in range(LAYERS):
        own_hidden = scaled(xf, norm_gain[layer], width)
        in_block = all_in[layer]
        partial_value = jnp.dot(own_hidden, in_block, preferred_element_type=jnp.float32).astype(
            jnp.bfloat16
        )
        upward = (
            lax.psum_scatter(partial_value, "tp", scatter_dimension=1, tiled=True)
            .astype(jnp.float32)
            .astype(jnp.bfloat16)
        )
        padded = padded_2(upward, (("sp", 0),), margin).astype(jnp.float32)
        sums = nested_sums(padded, tok_rows)
        wsum = sums[0]
        counted = jnp.broadcast_to(window_count(where, seq_len, 0)[:, None], (tok_rows, channels))
        for level in range(1, 4):
            chosen = (group_ids == level)[None, :]
            wsum = jnp.where(chosen, sums[level], wsum)
            counted = jnp.where(chosen, window_count(where, seq_len, level)[:, None], counted)
        pooled = (wsum / counted - upward.astype(jnp.float32)).astype(jnp.bfloat16)
        mapped = jnp.einsum(
            "tgc,gcd->tgd",
            pooled.reshape(tok_rows, groups_here, group_width),
            w_pool[layer],
            preferred_element_type=jnp.float32,
        )
        mixed = (mapped.reshape(tok_rows, channels) * pool_scale[layer][None, :]).astype(
            jnp.bfloat16
        )
        mixed_all = lax.all_gather(mixed, "tp", axis=1, tiled=True)
        output = jnp.dot(mixed_all, all_out[layer], preferred_element_type=jnp.float32)
        stored = (xf + output).astype(jnp.bfloat16)
        stored = lax.optimization_barrier(stored)
        xf = stored.astype(jnp.float32)
    return scaled(xf, final_gain, width)


MESH = pl.DeviceIdType.MESH


def fused(
    sp_size,
    resid_ref,
    gain_ref,
    final_ref,
    own_w,
    pool_ref,
    pscale_ref,
    out_ref,
    weights,
    xg,
    xcur,
    part_send,
    part_recv,
    uhalo,
    mixed,
    pool_all,
    pscale_all,
    ss_send,
    ss_recv,
    w_send_sem,
    w_recv_sem,
    x_send_sem,
    x_recv_sem,
    h_send_sem,
    h_recv_sem,
    s_send_sem,
    s_recv_sem,
    p_send_sem,
    p_recv_sem,
):
    depth = sp_size // 4
    rows = own_w.shape[1]
    tokens, width_here = resid_ref.shape
    groups, cg = pool_ref.shape[1], pool_ref.shape[2]
    total_groups = 2 * groups
    width = 2 * width_here
    edge = 2 * margin
    me = lax.axis_index("sp")
    t = lax.axis_index("tp")
    peer = 1 - t
    core = lax.rem(me, 2)
    y = lax.rem(me // 2, 2)
    z = me // 4

    def number(zz, yy, cc):
        return (zz * 2 + yy) * 2 + cc

    sibling = number(z, y, 1 - core)
    across = number(z, 1 - y, core)

    barrier = pltpu.get_barrier_semaphore()

    def greet(device):
        pl.semaphore_signal(barrier, inc=1, device_id=device, device_id_type=MESH)

    greet({"sp": sibling})
    greet({"sp": across})
    greet({"tp": peer})
    for ok, who in (
        (z > 0, me - 4),
        (z < depth - 1, me + 4),
        (z > 1, me - 8),
        (z < depth - 2, me + 8),
        (me > 0, me - 1),
        (me < sp_size - 1, me + 1),
    ):

        @pl.when(ok)
        def _(who=who):
            greet({"sp": who})

    expected = (
        3
        + jnp.where(z > 0, 1, 0)
        + jnp.where(z < depth - 1, 1, 0)
        + jnp.where(z > 1, 1, 0)
        + jnp.where(z < depth - 2, 1, 0)
        + jnp.where(me > 0, 1, 0)
        + jnp.where(me < sp_size - 1, 1, 0)
    )
    pl.semaphore_wait(barrier, expected)

    def landing(stage, piece):
        return weights.at[stage, pl.ds(pl.multiple_of(piece * rows, rows), rows), :]

    def hop(stage, zz, yy, way, target, from_own=False):
        piece = number(zz, yy, core)
        slot = {
            "sib": zz * 2 + yy,
            "y": 2 * depth + zz,
            "up1": 3 * depth + zz,
            "down1": 4 * depth + zz,
            "up2": 5 * depth,
            "down2": 5 * depth + 1,
            "pair": 5 * depth + 2,
        }[way]
        return pltpu.make_async_remote_copy(
            src_ref=own_w.at[stage] if from_own else landing(stage, piece),
            dst_ref=landing(stage, piece),
            send_sem=w_send_sem.at[stage, slot],
            recv_sem=w_recv_sem.at[stage, piece],
            device_id={"sp": target},
            device_id_type=MESH,
        )

    def wait_piece(stage, zz, yy, cc):
        piece = number(zz, yy, cc)
        pltpu.make_async_remote_copy(
            src_ref=landing(stage, piece),
            dst_ref=landing(stage, piece),
            send_sem=w_send_sem.at[stage, 0],
            recv_sem=w_recv_sem.at[stage, piece],
            device_id={"sp": sibling},
            device_id_type=MESH,
        ).wait_recv()

    def each_own(stage, act):
        for d in (1, 2):

            @pl.when(z + d < depth)
            def _(d=d):
                act(hop(stage, z, y, f"up{d}", me + 4 * d, True))

            @pl.when(z - d >= 0)
            def _(d=d):
                act(hop(stage, z, y, f"down{d}", me - 4 * d, True))

        act(hop(stage, z, y, "sib", sibling, True))

    def own_y(stage, act):
        act(hop(stage, z, y, "y", across, True))

    zpair = z + 1 - 2 * lax.rem(z, 2)
    by_pair = (core == 1) & (zpair < depth)

    def each_z(stage, d, act, arrive):
        @pl.when(z - d >= 0)
        def _():
            if arrive:
                wait_piece(stage, z - d, y, core)
            if d >= 2:

                @pl.when(z < depth - 1)
                def _():
                    act(hop(stage, z - d, y, "up1", me + 4))

            if d > 1:
                act(hop(stage, z - d, y, "y", across))
            else:

                @pl.when(jnp.logical_not(by_pair & (zpair == z - 1)))
                def _():
                    act(hop(stage, z - 1, y, "y", across))

            act(hop(stage, z - d, y, "sib", sibling))

        @pl.when(z + d < depth)
        def _():
            if arrive:
                wait_piece(stage, z + d, y, core)
            if d >= 2:

                @pl.when(z > 0)
                def _():
                    act(hop(stage, z + d, y, "down1", me - 4))

            if d > 1:
                act(hop(stage, z + d, y, "y", across))
            else:

                @pl.when(jnp.logical_not(by_pair & (zpair == z + 1)))
                def _():
                    act(hop(stage, z + 1, y, "y", across))

            act(hop(stage, z + d, y, "sib", sibling))

    def each_y(stage, d, act, arrive):
        def one(zz):
            if arrive:
                wait_piece(stage, zz, 1 - y, core)
            act(hop(stage, zz, 1 - y, "sib", sibling))

        if d == 0:
            one(z)

            @pl.when(by_pair)
            def _():
                act(hop(stage, z, 1 - y, "pair", number(zpair, y, core)))

        else:

            @pl.when(z - d >= 0)
            def _():
                one(z - d)

            @pl.when(z + d < depth)
            def _():
                one(z + d)

    begin = lambda copy: copy.start()
    drain = lambda copy: copy.wait_send()

    def step_own(stage):
        if stage < 2 * LAYERS:
            each_own(stage, begin)
        if stage + 1 < 2 * LAYERS:
            own_y(stage + 1, begin)

    def step_z(stage, d):
        if stage < 2 * LAYERS and d < depth:
            each_z(stage, d, begin, True)

    def step_y(stage, d):
        if stage < 2 * LAYERS and d < depth:
            each_y(stage, d, begin, True)

    def opening(stage):
        step_y(stage, 0)
        step_z(stage, 2)
        step_own(stage + 2)
        step_y(stage, 1)

    def closing(stage, ahead=True):
        for d in range(3, depth):
            step_z(stage, d)
        if ahead:
            step_z(stage + 1, 1)
        for d in range(2, depth):
            step_y(stage, d)
        if not ahead:
            step_z(stage + 1, 1)

    def settle(stage):
        for zz in range(depth):
            for yy in range(2):
                wait_piece(stage, zz, yy, 1 - core)

    def finish(stage):
        each_own(stage, drain)
        own_y(stage, drain)
        for d in range(1, depth):
            each_z(stage, d, drain, False)
        for d in range(depth):
            each_y(stage, d, drain, False)

    diagonal = lax.broadcasted_iota(jnp.int32, (tokens, tokens), 0) == lax.broadcasted_iota(
        jnp.int32, (tokens, tokens), 1
    )

    def send_squares(k):
        return pltpu.make_async_remote_copy(
            src_ref=ss_send.at[k],
            dst_ref=ss_recv.at[k],
            send_sem=s_send_sem.at[k],
            recv_sem=s_recv_sem.at[k],
            device_id={"tp": peer},
            device_id_type=MESH,
        )

    def store_squares(k, column):
        line = jnp.sum(jnp.where(diagonal, column, 0.0), axis=0, keepdims=True)
        ss_send[k] = jnp.broadcast_to(line, ss_send.shape[1:])

    def norm_factor(k):
        send_squares(k).wait_recv()
        line = ss_send[k][0:1, :] + ss_recv[k][0:1, :]
        column = jnp.sum(jnp.where(diagonal, line, 0.0), axis=1, keepdims=True)
        return lax.rsqrt(column / width + eps)

    def x_copy(layer, j):
        k = layer * total_groups + j
        return pltpu.make_async_remote_copy(
            src_ref=part_send.at[layer, j],
            dst_ref=part_recv.at[layer, j],
            send_sem=x_send_sem.at[k],
            recv_sem=x_recv_sem.at[k],
            device_id={"tp": peer},
            device_id_type=MESH,
        )

    def pool_copy(layer):
        return pltpu.make_async_remote_copy(
            src_ref=pool_ref.at[layer] if layer < LAYERS else pscale_ref,
            dst_ref=pool_all.at[layer, t] if layer < LAYERS else pscale_all.at[t],
            send_sem=p_send_sem.at[layer],
            recv_sem=p_recv_sem.at[layer],
            device_id={"tp": peer},
            device_id_type=MESH,
        )

    def halo(layer, j, upward):
        if upward:
            source = uhalo.at[layer, j, pl.ds(tokens, edge), :]
            target = uhalo.at[layer, j, pl.ds(0, edge), :]
        else:
            source = uhalo.at[layer, j, pl.ds(edge, edge), :]
            target = uhalo.at[layer, j, pl.ds(edge + tokens, edge), :]
        k = (layer * total_groups + j) * 2 + (1 if upward else 0)
        return pltpu.make_async_remote_copy(
            src_ref=source,
            dst_ref=target,
            send_sem=h_send_sem.at[k],
            recv_sem=h_recv_sem.at[k],
            device_id={"sp": me + 1 if upward else me - 1},
            device_id_type=MESH,
        )

    def each_halo(layer, j, act):
        @pl.when(me < sp_size - 1)
        def _():
            act(halo(layer, j, True))

        @pl.when(me > 0)
        def _():
            act(halo(layer, j, False))

    def inward(layer, d):
        def plane(zz):
            for yy in range(2):
                wait_piece(2 * layer, zz, yy, 1 - core)
            block = weights[2 * layer, pl.ds(pl.multiple_of(zz * cg, cg), cg), :]
            part = lax.dot_general(
                xg[...], block, (((1,), (1,)), ((), ())), preferred_element_type=jnp.float32
            )
            part_send[layer, zz] = part.astype(jnp.bfloat16)
            x_copy(layer, zz).start()

        if d == 0:
            plane(z)
        else:

            @pl.when(z - d >= 0)
            def _():
                plane(z - d)

            @pl.when(z + d < depth)
            def _():
                plane(z + d)

    def closing_inward(layer):
        stage = 2 * layer
        inward(layer, 0)
        for d in range(3, depth):
            step_z(stage, d)
        if layer > 0:
            step_z(stage + 1, 1)
        inward(layer, 1)
        for d in range(2, depth):
            step_y(stage, d)
            inward(layer, d)
        if layer == 0:
            step_z(stage + 1, 1)

    def pooling(layer):
        factor = norm_factor(layer)
        pool_copy(layer).wait_recv()
        if layer == 0:
            pool_copy(LAYERS).wait_recv()
        for j in range(total_groups):
            x_copy(layer, j).wait_recv()
            value = part_send[layer, j].astype(jnp.float32) + part_recv[layer, j].astype(jnp.float32)
            uhalo[layer, j, pl.ds(edge, tokens), :] = (value * factor).astype(jnp.bfloat16)
            each_halo(layer, j, begin)
        row = lax.broadcasted_iota(jnp.int32, (tokens, tokens + 2 * edge), 0)
        col = lax.broadcasted_iota(jnp.int32, (tokens, tokens + 2 * edge), 1) - edge
        where = me * tokens + lax.broadcasted_iota(jnp.int32, (tokens, 1), 0)
        seq_len = tokens * sp_size
        for j in range(total_groups):
            left = 2**j
            band = jnp.where((col >= row - left) & (col <= row + left - 1), 1.0, 0.0).astype(
                jnp.bfloat16
            )
            upper = jnp.minimum(where + left, seq_len)
            lower = jnp.maximum(where - left, 0)
            inverse = 1.0 / (upper - lower).astype(jnp.float32)

            @pl.when(me > 0)
            def _(j=j):
                halo(layer, j, True).wait_recv()

            @pl.when(me < sp_size - 1)
            def _(j=j):
                halo(layer, j, False).wait_recv()

            wsum = jnp.dot(band, uhalo[layer, j], preferred_element_type=jnp.float32)
            pooled = wsum * inverse - uhalo[layer, j, pl.ds(edge, tokens), :].astype(jnp.float32)
            mapped = jnp.dot(
                pooled.astype(jnp.bfloat16), pool_all[layer, j // groups, j % groups], preferred_element_type=jnp.float32
            )
            first = j % groups * cg
            scale = pscale_all[j // groups, layer : layer + 1, first : first + cg]
            mixed[j] = (mapped * scale).astype(jnp.bfloat16)

    step = cg

    def outward(layer):
        squares = jnp.zeros((tokens, 1), jnp.float32)
        for n in range(0, width_here, step):
            total = xcur[:, n : n + step].astype(jnp.float32)
            for j in range(total_groups):
                block = weights[2 * layer + 1, j * cg : (j + 1) * cg, n : n + step]
                total = total + jnp.dot(mixed[j], block, preferred_element_type=jnp.float32)
            stored = total.astype(jnp.bfloat16)
            xcur[:, n : n + step] = stored
            value = stored.astype(jnp.float32)
            squares = squares + jnp.sum(value * value, axis=1, keepdims=True)
            if layer + 1 < LAYERS:
                xg[:, n : n + step] = (
                    value * gain_ref[layer + 1 : layer + 2, n : n + step]
                ).astype(jnp.bfloat16)
        store_squares(layer + 1, squares)

    for k in range(LAYERS + 1):
        pool_copy(k).start()
    own_y(0, begin)
    step_own(0)
    step_own(1)
    squares = jnp.zeros((tokens, 1), jnp.float32)
    for n in range(0, width_here, step):
        value = resid_ref[:, n : n + step].astype(jnp.float32)
        squares = squares + jnp.sum(value * value, axis=1, keepdims=True)
        xcur[:, n : n + step] = resid_ref[:, n : n + step]
        xg[:, n : n + step] = (value * gain_ref[0:1, n : n + step]).astype(jnp.bfloat16)
    store_squares(0, squares)
    pool_all[:, pl.ds(t, 1)] = pool_ref[...][:, None]
    pscale_all[pl.ds(t, 1)] = pscale_ref[...][None]
    nothing = jnp.zeros((LAYERS, total_groups, edge, cg), jnp.bfloat16)

    @pl.when(me == 0)
    def _():
        uhalo[:, :, pl.ds(0, edge), :] = nothing

    @pl.when(me == sp_size - 1)
    def _():
        uhalo[:, :, pl.ds(edge + tokens, edge), :] = nothing

    for stage in range(2 * LAYERS):
        weights[stage, pl.ds(pl.multiple_of(me * rows, rows), rows), :] = own_w[stage]
    send_squares(0).start()

    step_z(0, 1)
    opening(0)
    for layer in range(LAYERS):
        closing_inward(layer)
        opening(2 * layer + 1)
        closing(2 * layer + 1)
        pooling(layer)
        if layer + 1 < LAYERS:
            opening(2 * layer + 2)
        settle(2 * layer + 1)
        outward(layer)
        send_squares(layer + 1).start()
    for stage in range(2 * LAYERS):
        finish(stage)
    for k in range(LAYERS + 1):
        pool_copy(k).wait_send()
    for layer in range(LAYERS):
        for j in range(total_groups):
            x_copy(layer, j).wait_send()
            each_halo(layer, j, drain)

    factor = norm_factor(LAYERS)
    for n in range(0, width_here, step):
        out_ref[:, n : n + step] = (
            xcur[:, n : n + step].astype(jnp.float32) * factor * final_ref[0:1, n : n + step]
        ).astype(jnp.bfloat16)
    for k in range(LAYERS + 1):
        send_squares(k).wait_send()


def one_kernel(resid, norm_gain, w_in, w_pool, pool_scale, w_out, final_gain):
    sp_size = lax.axis_size("sp")
    depth = sp_size // 4
    tokens, width_here = resid.shape
    rows = w_out.shape[1]
    groups, cg = w_pool.shape[1], w_pool.shape[2]
    edge = 2 * margin
    turned = jnp.swapaxes(w_in, 1, 2)
    pieces = jnp.stack([turned, w_out], axis=1).reshape(2 * LAYERS, rows, width_here)
    vmem = pl.BlockSpec(memory_space=pltpu.VMEM)
    bf, f32 = jnp.bfloat16, jnp.float32
    dma = pltpu.SemaphoreType.DMA
    crossing = pltpu.VMEM((LAYERS, 2 * groups, tokens, cg), bf)
    return pl.pallas_call(
        functools.partial(fused, sp_size),
        out_shape=jax.ShapeDtypeStruct(resid.shape, bf),
        in_specs=[vmem] * 6,
        out_specs=vmem,
        scratch_shapes=[
            pltpu.VMEM((2 * LAYERS, sp_size * rows, width_here), bf),
            pltpu.VMEM((tokens, width_here), bf),
            pltpu.VMEM((tokens, width_here), bf),
            crossing,
            crossing,
            pltpu.VMEM((LAYERS, 2 * groups, tokens + 2 * edge, cg), bf),
            pltpu.VMEM((2 * groups, tokens, cg), bf),
            pltpu.VMEM((LAYERS, 2, groups, cg, cg), bf),
            pltpu.VMEM((2, LAYERS, groups * cg), f32),
            pltpu.VMEM((LAYERS + 1, 8, tokens), f32),
            pltpu.VMEM((LAYERS + 1, 8, tokens), f32),
            dma((2 * LAYERS, 5 * depth + 3)),
            dma((2 * LAYERS, sp_size)),
            dma((4 * LAYERS * groups,)),
            dma((4 * LAYERS * groups,)),
            dma((4 * LAYERS * groups,)),
            dma((4 * LAYERS * groups,)),
            dma((LAYERS + 1,)),
            dma((LAYERS + 1,)),
            dma((LAYERS + 1,)),
            dma((LAYERS + 1,)),
        ],
        compiler_params=pltpu.CompilerParams(
            collective_id=0, has_side_effects=True, vmem_limit_bytes=48 * 2**20
        ),
    )(resid, norm_gain, final_gain[None, :], pieces, w_pool, pool_scale)


def spread(*args):
    resid, w_pool, w_out = args[0], args[3], args[5]
    fits = (
        lax.axis_size("tp") == 2
        and lax.axis_size("sp") % 4 == 0
        and w_out.shape[1] % 16 == 0
        and 4 * w_out.shape[1] == w_pool.shape[2]
        and lax.axis_size("sp") // 4 == 2 * w_pool.shape[1]
        and resid.shape[0] % 128 == 0
        and w_pool.shape[2] % 128 == 0
        and resid.shape[1] % w_pool.shape[2] == 0
    )
    return one_kernel(*args) if fits else shards(*args)


def solution(mesh):
    placed = (
        P("sp", "tp"),
        P(None, "tp"),
        P(None, "tp", "sp"),
        P(None, "tp", None, None),
        P(None, "tp"),
        P(None, "sp", "tp"),
        P("tp"),
    )
    return jax.shard_map(
        spread, mesh=mesh, in_specs=placed, out_specs=P("sp", "tp"), check_vma=False
    )
```
